32 devices in a mesh: rep: 2 (over x), fs: 4 (over z), tp: 4 (over y, core).
Axes of the slice: x: 2, y: 2, z: 4, core: 2. Of those that a mesh axis runs over, the one named last changes fastest.
Arguments:
- tokens: bfloat16 [6144, 2048], P(('rep', 'fs'), 'tp'), may hold values from -6 to 6
- gain_mix: bfloat16 [2048], replicated, may hold values from 0.099609375 to 1.8984375
- query_weight: bfloat16 [2048, 1024], P('fs', 'tp'), may hold values from -0.125 to 0.125
- key_weight: bfloat16 [2048, 1024], P('fs', 'tp'), may hold values from -0.125 to 0.125
- value_weight: bfloat16 [2048, 2048], P('fs', 'tp'), may hold values from -0.125 to 0.125
- gate_weight: bfloat16 [2048, 2048], P('fs', 'tp'), may hold values from -0.125 to 0.125
- decay_rate: float32 [8], P('tp'), may hold values from 0.0006510417 to 0.05
- out_weight: bfloat16 [2048, 2048], P('tp', 'fs'), may hold values from -0.125 to 0.125
- gain_mlp: bfloat16 [2048], replicated, may hold values from 0.099609375 to 1.8984375
- up_weight: bfloat16 [2048, 8192], P('fs', 'tp'), may hold values from -0.125 to 0.125
- down_weight: bfloat16 [8192, 2048], P('tp', 'fs'), may hold values from -0.0625 to 0.0625
Outputs:
- layer_out: bfloat16 [6144, 2048], P(('rep', 'fs'), 'tp')
The draws below stay inside these ranges and needn't reach their ends.
All inputs are finite; a program needn't handle non-finite values.
Results may differ from the reference program's by a relative error of at most 0.019.
Values may be sent and summed in bfloat16 or wider, within the bound.
A program may use at most 128 MiB of HBM per device.

```python
import math
import jax
import jax.numpy as jnp
from jax import lax

D = 2048
HEADS = 8
DK = 128
DV = 256
FF = 8192
SEQ = 768
BLK = 128
TOKENS = 6144
N_TP = 4


def steps_of(rng, shape, pieces, low, top_value):
    level, own = 1.0, jax.random.fold_in(rng, 6)
    for dim, shards_of in pieces:
        heights = jnp.exp(jax.random.uniform(jax.random.fold_in(own, dim), (shards_of,), jnp.float32, low / len(pieces), top_value / len(pieces)))
        level = level * jnp.repeat(heights, shape[dim] // shards_of).reshape([-1 if axis == dim else 1 for axis in range(len(shape))])
    return level


def centred(own_key, dims, spread, bound, split=(), held_as=jnp.bfloat16):
    entries = spread * jax.random.normal(own_key, dims, jnp.float32)
    if split:
        entries = entries * steps_of(own_key, dims, split, -0.22, 0.18)
    return jnp.clip(entries, -bound, bound).astype(held_as)


def setup_inputs(seed: int = 0) -> dict:
    key_list = jax.random.split(jax.random.key(seed), 12)
    tokens = centred(key_list[0], (TOKENS, D), 1.0, 6.0, ((0, 8), (1, 4)))
    gain_mix = jnp.clip(1.0 + 0.18 * jax.random.normal(key_list[1], (D,), jnp.float32), 0.099609375, 1.8984375).astype(jnp.bfloat16)
    query_weight = centred(key_list[2], (D, HEADS * DK), D ** -0.5, 0.125, ((0, 4), (1, 4)))
    key_weight = centred(key_list[3], (D, HEADS * DK), D ** -0.5, 0.125, ((0, 4), (1, 4)))
    value_weight = centred(key_list[4], (D, HEADS * DV), D ** -0.5, 0.125, ((0, 4), (1, 4)))
    gate_weight = centred(key_list[5], (D, HEADS * DV), D ** -0.5, 0.125, ((0, 4), (1, 4)))
    decay_rate = jnp.clip(jnp.exp(math.log(0.05) - 4.3412046 * jax.random.uniform(key_list[6], (HEADS,), jnp.float32) ** steps_of(key_list[6], (HEADS,), ((0, 4),), -0.2, 0.2)), 0.0006510417, 0.05)
    out_weight = centred(key_list[7], (HEADS * DV, D), (HEADS * DV) ** -0.5, 0.125, ((0, 4), (1, 4)))
    gain_mlp = jnp.clip(1.0 + 0.18 * jax.random.normal(key_list[8], (D,), jnp.float32), 0.099609375, 1.8984375).astype(jnp.bfloat16)
    up_weight = centred(key_list[9], (D, FF), D ** -0.5, 0.125, ((0, 4), (1, 4)))
    down_weight = centred(key_list[10], (FF, D), FF ** -0.5, 0.0625, ((0, 4), (1, 4)))
    return dict(tokens=tokens, gain_mix=gain_mix, query_weight=query_weight, key_weight=key_weight, value_weight=value_weight, gate_weight=gate_weight, decay_rate=decay_rate, out_weight=out_weight, gain_mlp=gain_mlp, up_weight=up_weight, down_weight=down_weight)


epsilon = 1e-06
highest = lax.Precision.HIGHEST

def rms_rows(rows, gain):
    values = rows.astype(jnp.float32)
    scaled = values * lax.rsqrt(lax.optimization_barrier(jnp.mean(values * values, axis=-1, keepdims=True)) + epsilon)
    return (scaled * gain.astype(jnp.float32)).astype(jnp.bfloat16)

def retain(query, keys, values, rate, block):
    length, head_count, key_width = query.shape
    value_width = values.shape[-1]
    block_count = length // block
    log_decay = -rate.astype(jnp.float32)
    positions = jnp.arange(block, dtype=jnp.float32)
    distance = positions[:, None] - positions[None, :]
    causal = distance >= 0
    inside = jnp.where(causal[None], jnp.exp(log_decay[:, None, None] * jnp.where(causal, distance, 0.0)[None]), 0.0)
    key_scale = jnp.exp(log_decay[None, :] * (block - 1.0 - positions)[:, None])
    query_scale = jnp.exp(log_decay[None, :] * (positions + 1.0)[:, None])
    carry_decay = jnp.exp(log_decay * block)
    query_blocks = query.reshape(block_count, block, head_count, key_width)
    key_blocks = keys.reshape(block_count, block, head_count, key_width) * key_width ** (-0.5)
    value_blocks = values.reshape(block_count, block, head_count, value_width)

    def advance(state, blocks):
        q_block, k_block, v_block = blocks
        scores = jnp.einsum('ihd,jhd->hij', q_block, k_block, precision=highest) * inside
        inner = jnp.einsum('hij,jhe->ihe', scores, v_block, precision=highest)
        cross = jnp.einsum('ihd,hde->ihe', q_block, state, precision=highest) * query_scale[:, :, None]
        update = jnp.einsum('jhd,jhe->hde', k_block * key_scale[:, :, None], v_block, precision=highest)
        return (state * carry_decay[:, None, None] + update, inner + cross)
    initial = jnp.zeros((head_count, key_width, value_width), jnp.float32)
    _, results = lax.scan(advance, initial, (query_blocks, key_blocks, value_blocks))
    return results.reshape(length, head_count, value_width)

def gated_heads(retained, gate):
    length, head_count, value_width = retained.shape
    normed = retained * lax.rsqrt(lax.optimization_barrier(jnp.mean(retained * retained, axis=-1, keepdims=True)) + epsilon)
    gated = jax.nn.silu(gate.reshape(length, head_count, value_width)) * normed
    return gated.reshape(length, head_count * value_width).astype(jnp.bfloat16)

def grouped_sum(left, right, groups):
    rows = left.shape[0]
    inner_width = left.shape[1] // groups
    left_groups = left.reshape(rows, groups, inner_width).astype(jnp.float32)
    right_groups = right.reshape(groups, inner_width, right.shape[1]).astype(jnp.float32)
    parts = jnp.einsum('sgc,gcd->gsd', left_groups, right_groups)
    rounded = lax.optimization_barrier(parts.astype(jnp.bfloat16)).astype(jnp.float32)
    return lax.optimization_barrier(jnp.sum(rounded, axis=0))

def reference(tokens, gain_mix, query_weight, key_weight, value_weight, gate_weight, decay_rate, out_weight, gain_mlp, up_weight, down_weight):

    def one_sequence(rows):
        normed = rms_rows(rows, gain_mix)
        query = jnp.dot(normed, query_weight, preferred_element_type=jnp.float32).reshape(SEQ, HEADS, DK)
        keys = jnp.dot(normed, key_weight, preferred_element_type=jnp.float32).reshape(SEQ, HEADS, DK)
        values = jnp.dot(normed, value_weight, preferred_element_type=jnp.float32).reshape(SEQ, HEADS, DV)
        gate = jnp.dot(normed, gate_weight, preferred_element_type=jnp.float32)
        retained = retain(query, keys, values, decay_rate, BLK)
        hidden = gated_heads(retained, gate)
        mixed = (rows.astype(jnp.float32) + grouped_sum(hidden, out_weight, N_TP)).astype(jnp.bfloat16)
        normed_mlp = rms_rows(mixed, gain_mlp)
        upward = jnp.dot(normed_mlp, up_weight, preferred_element_type=jnp.float32)
        active = jnp.square(jax.nn.relu(upward)).astype(jnp.bfloat16)
        return (mixed.astype(jnp.float32) + grouped_sum(active, down_weight, N_TP)).astype(jnp.bfloat16)
    sequences = tokens.reshape(TOKENS // SEQ, SEQ, D)
    return lax.map(one_sequence, sequences).reshape(TOKENS, D)
```

```python
import jax
import jax.numpy as jnp
from jax import lax
from jax.sharding import PartitionSpec as P


DK = 128
DV = 256
EPS = 1e-06

ORDER = (2, 1, 3)


def rms_rows(rows, gain):
    values = rows.astype(jnp.float32)
    scaled = values * lax.rsqrt(jnp.mean(values * values, axis=-1, keepdims=True) + EPS)
    return (scaled * gain.astype(jnp.float32)).astype(jnp.bfloat16)


def shift(x, axis, n, by):
    return lax.ppermute(x, axis, [(k, (k + by) % n) for k in range(n)])


def far_pieces(chunk, n):
    if n != 4:
        return [shift(chunk, "fs", n, s) for s in range(1, n)]
    me = lax.axis_index("fs")
    two = lax.ppermute(chunk, "fs", [(0, 2), (1, 3), (2, 0), (3, 1)])
    left = lax.ppermute(chunk, "fs", [(0, 1), (1, 2), (2, 3)])
    right = lax.ppermute(chunk, "fs", [(1, 0), (2, 1), (3, 2)])
    ends = lax.ppermute(two, "fs", [(1, 0), (2, 3)])
    return [jnp.where(me == 0, ends, left), two, jnp.where(me == 3, ends, right)]


def gather(weight, dim, n, reps):
    width = weight.shape[dim]
    me = lax.axis_index("fs")
    starts = [lax.rem(me - s + n, n) * width for s in range(n)]
    if reps != 2:
        return list(zip([weight] + far_pieces(weight, n), starts))
    p = lax.axis_index("rep")
    half = width // 2
    mine = far_pieces(lax.dynamic_slice_in_dim(weight, p * half, half, axis=dim), n)
    pieces = [(weight, starts[0])]
    for s in ORDER if n == 4 else range(1, n):
        other = shift(mine[s - 1], "rep", 2, 1)
        pieces.append((mine[s - 1], starts[s] + p * half))
        pieces.append((other, starts[s] + (1 - p) * half))
    return pieces


def assemble(pieces, dim, width):
    shape = list(pieces[0][0].shape)
    shape[dim] = width
    out = jnp.zeros(shape, pieces[0][0].dtype)
    for piece, start in pieces:
        out = lax.dynamic_update_slice_in_dim(out, piece, start, axis=dim)
    return out


def product(left, right):
    return jnp.dot(left, right, preferred_element_type=jnp.float32)


def core_swap(x, n):
    return lax.ppermute(x, "tp", [(k, k ^ 1) for k in range(n)])


def gather_features(block, n):
    rows, width = block.shape
    me = lax.axis_index("tp")
    other = me + 1 - 2 * lax.rem(me, 2)
    out = jnp.zeros((rows, width * n), block.dtype)
    out = lax.dynamic_update_slice_in_dim(out, block, me * width, axis=1)
    out = lax.dynamic_update_slice_in_dim(out, core_swap(block, n), other * width, axis=1)
    for d in range(2, n, 2):
        far = shift(block, "tp", n, d)
        near = core_swap(far, n)
        out = lax.dynamic_update_slice_in_dim(out, far, lax.rem(me - d + n, n) * width, axis=1)
        out = lax.dynamic_update_slice_in_dim(out, near, lax.rem(other - d + n, n) * width, axis=1)
    return out


def scatter_sum(terms, n):
    width = terms.shape[1] // n
    me = lax.axis_index("tp")
    other = me + 1 - 2 * lax.rem(me, 2)
    total = None
    for d in list(range(2, n, 2)) + [0]:
        mine = lax.dynamic_slice_in_dim(terms, lax.rem(me + d, n) * width, width, axis=1)
        theirs = lax.dynamic_slice_in_dim(terms, lax.rem(other + d, n) * width, width, axis=1)
        pair = mine.astype(jnp.float32) + core_swap(theirs, n).astype(jnp.float32)
        if d:
            pair = shift(pair.astype(jnp.bfloat16), "tp", n, d).astype(jnp.float32)
        total = pair if total is None else total + pair
    return total


def retain(query, keys, values, rate):
    length, heads, _ = query.shape
    positions = jnp.arange(length, dtype=jnp.float32)
    distance = positions[:, None] - positions[None, :]
    causal = distance >= 0
    outs = []
    for h in range(heads):
        decay = jnp.where(causal, jnp.exp(-rate[h] * jnp.where(causal, distance, 0.0)), 0.0)
        scores = jnp.einsum(
            "id,jd->ij", query[:, h], keys[:, h], preferred_element_type=jnp.float32
        )
        scores = (scores * (DK ** -0.5) * decay).astype(jnp.bfloat16)
        outs.append(jnp.dot(scores, values[:, h], preferred_element_type=jnp.float32))
    return jnp.stack(outs, axis=1)


def gated_heads(retained, gate):
    length, heads, width = retained.shape
    normed = retained * lax.rsqrt(jnp.mean(retained * retained, axis=-1, keepdims=True) + EPS)
    gated = jax.nn.silu(gate.reshape(length, heads, width)) * normed
    return gated.reshape(length, heads * width).astype(jnp.bfloat16)


def solution(mesh):
    n_fs, n_tp, n_rep = mesh.shape["fs"], mesh.shape["tp"], mesh.shape["rep"]

    def layer(
        tokens, gain_mix, query_weight, key_weight, value_weight, gate_weight,
        decay_rate, out_weight, gain_mlp, up_weight, down_weight,
    ):
        length = tokens.shape[0]
        width = tokens.shape[1] * n_tp
        heads = decay_rate.shape[0]
        whole = gather_features(tokens, n_tp)
        first = jnp.concatenate([query_weight, key_weight, value_weight, gate_weight], axis=1)
        first_parts = gather(first, 0, n_fs, n_rep)
        out_parts = gather(out_weight, 1, n_fs, n_rep)
        up_parts = gather(up_weight, 0, n_fs, n_rep)
        down_parts = gather(down_weight, 1, n_fs, n_rep)

        normed = rms_rows(whole, gain_mix)
        qkvg = product(normed, assemble(first_parts, 0, width))
        a, b, c = heads * DK, 2 * heads * DK, 2 * heads * DK + heads * DV
        low = qkvg[:, :c].astype(jnp.bfloat16)
        retained = retain(
            low[:, :a].reshape(length, heads, DK),
            low[:, a:b].reshape(length, heads, DK),
            low[:, b:c].reshape(length, heads, DV),
            decay_rate,
        )
        hidden = gated_heads(retained, qkvg[:, c:])
        mix_terms = product(hidden, assemble(out_parts, 1, width)).astype(jnp.bfloat16)
        mixed = (tokens.astype(jnp.float32) + scatter_sum(mix_terms, n_tp)).astype(jnp.bfloat16)
        normed_mlp = rms_rows(gather_features(mixed, n_tp), gain_mlp)
        upward = product(normed_mlp, assemble(up_parts, 0, width))
        active = jnp.square(jax.nn.relu(upward)).astype(jnp.bfloat16)
        mlp_terms = product(active, assemble(down_parts, 1, width)).astype(jnp.bfloat16)
        return (mixed.astype(jnp.float32) + scatter_sum(mlp_terms, n_tp)).astype(jnp.bfloat16)

    return jax.shard_map(
        layer,
        mesh=mesh,
        in_specs=(
            P(("rep", "fs"), "tp"), P(), P("fs", "tp"), P("fs", "tp"), P("fs", "tp"),
            P("fs", "tp"), P("tp"), P("tp", "fs"), P(), P("fs", "tp"), P("tp", "fs"),
        ),
        out_specs=P(("rep", "fs"), "tp"),
        check_vma=False,
    )
```
